32 devices in a mesh: ep: 8 (over z, core), tp: 4 (over y, x).
Axes of the slice: x: 2, y: 2, z: 4, core: 2. Of those that a mesh axis runs over, the one named last changes fastest.
Arguments:
- tokens: bfloat16 [128, 4096], P('ep', 'tp'), may hold values from -40 to 40
- norm_gain: bfloat16 [4096], P('tp'), may hold values from 0.099609375 to 1.8984375
- routes: int32 [128, 4], P('ep'), may hold values from 0 to 7, all different within a row; in each aligned block of 16 rows (0 to 15, 16 to 31, ...) at most 16 rows name the same one
- route_weights: float32 [128, 4], P('ep'), may hold values from 0.05 to 1
- w_gate: bfloat16 [8, 4096, 4096], P('ep', None, 'tp'), may hold values from -0.25 to 0.25
- w_up: bfloat16 [8, 4096, 4096], P('ep', None, 'tp'), may hold values from -0.25 to 0.25
- w_down: bfloat16 [8, 4096, 4096], P('ep', 'tp'), may hold values from -0.0234375 to 0.0234375
Outputs:
- mixed: bfloat16 [128, 4096], P('ep', 'tp')
The draws below stay inside these ranges and needn't reach their ends.
Inputs may be any that keep to these rules, and one draw needn't show every extreme that they name: `routes`: within the 16 rows of one device, each token names 4 different experts, and no expert is named by more than 16 rows; some expert reaches 16.
All inputs are finite; a program needn't handle non-finite values.
Results may differ from the reference program's by a relative error of at most 0.018.
Values may be sent and summed in bfloat16 or wider, within the bound.
A program may use at most 64 MiB of HBM per device.

```python
import math
import jax
import jax.numpy as jnp
import numpy as np
from jax import lax

D = 4096
FF = 4096
TOPK = 4
TOK_DEV = 16
EXPERTS = 8
CAP = 16
TOKENS = 128
N_TP = 4


def draw_tokens(key, part):
    first, second, third = jax.random.split(key, 3)
    blocks = max(D // 128, 1)
    width = D // blocks
    column_scale = jnp.exp(jax.random.uniform(second, (blocks,), jnp.float32, -1.1, 1.1))
    column_scale = jnp.repeat(column_scale, width)
    values = jax.random.normal(first, (TOKENS, D), jnp.float32) * column_scale[None, :]
    return jnp.clip(values, -40.0, 40.0).astype(jnp.bfloat16)


def level_of(stream_key, extent, cuts, smallest, top_value):
    level, own = 1.0, jax.random.fold_in(stream_key, 6)
    for axis_at, shards_of in cuts:
        heights = jnp.exp(jax.random.uniform(jax.random.fold_in(own, axis_at), (shards_of,), jnp.float32, smallest / len(cuts), top_value / len(cuts)))
        level = level * jnp.repeat(heights, extent[axis_at] // shards_of).reshape([-1 if axis == axis_at else 1 for axis in range(len(extent))])
    return level


def assign_block(rng, own, number, rows, number_of, top, bound, lean):
    sequence = jax.random.permutation(rng, number_of)
    heavy_load, usual = shares(number_of, rows * top, bound, lean, True), shares(number_of, rows * top, bound, lean, False)
    places = jnp.arange(number_of)

    def named(tallies, turn):
        used = int((tallies > 0).sum())
        fixed = max(1, used // 4)
        moved = fixed + (places - fixed + turn * (used - fixed)) % max(1, number_of - fixed)
        return jnp.zeros((number_of,), jnp.int32).at[sequence[jnp.where(places < fixed, places, moved)]].set(jnp.asarray(tallies, jnp.int32))

    tallies = jnp.where(number % 4 == 0, named(heavy_load, number // 4), named(usual, number - number // 4 - 1))
    mixed = jax.random.permutation(jax.random.fold_in(own, 3), number_of)
    giver, sink = mixed[0:number_of // 2 * 2:2], mixed[1:number_of // 2 * 2:2]
    slack = jnp.minimum(tallies[giver] - 1, bound - tallies[sink]) // 2
    slack = jnp.where((giver == sequence[0]) | (sink == sequence[0]) | (tallies[sink] == 0), 0, jnp.maximum(slack, 0))
    moved = jax.random.randint(jax.random.fold_in(own, 4), (number_of // 2,), 0, 1 << 20) % (slack + 1)
    tallies = tallies.at[giver].add(-moved).at[sink].add(moved)
    labels = jnp.searchsorted(jnp.cumsum(tallies), jnp.arange(rows * top), side="right").astype(jnp.int32)
    table = labels.reshape(top, rows).T
    table = table[jax.random.permutation(jax.random.fold_in(own, 1), rows)]
    turn = jax.random.randint(jax.random.fold_in(own, 2), (rows, 1), 0, top)
    return jnp.take_along_axis(table, (jnp.arange(top)[None, :] + turn) % top, axis=1)


def shares(count, total, limit, skew, full):
    portions = [(1 << 20) // math.isqrt(grade ** skew) + 1 for grade in range(1, count + 1)]
    largest = limit if full else min(limit, max(-(-total // count), total * portions[0] // sum(portions)))
    least = 1 if total - largest >= count - 1 else 0
    holding, rest = [largest] + [least] * (count - 1), total - largest - least * (count - 1)
    while rest > 0:
        free = [i for i in range(1, count) if holding[i] < largest] or [i for i in range(1, count) if holding[i] < limit]
        mass, remaining = sum([portions[i] for i in free]), rest
        for i in free:
            addition = min(limit - holding[i], max(1, remaining * portions[i] // mass), rest)
            holding[i] = holding[i] + addition
            rest = rest - addition
    return np.array(holding)


def scatter_about(own_key, extent, deviation, reach, cuts=(), held_as=jnp.bfloat16):
    array = jax.random.normal(own_key, extent, jnp.float32) * deviation
    if len(cuts) > 0:
        array = level_of(own_key, extent, cuts, -0.22, 0.18) * array
    return jnp.clip(array, min=-reach, max=reach).astype(held_as)


def setup_inputs(seed: int = 0) -> dict:
    arg_keys = jax.random.split(jax.random.key(seed), 8)
    tokens = draw_tokens(jax.random.fold_in(arg_keys[7], 71), 0)
    norm_gain = jnp.clip(1.0 + 0.18 * jax.random.normal(arg_keys[1], (D,), jnp.float32), 0.099609375, 1.8984375).astype(jnp.bfloat16)
    routes_keys = jax.random.split(jax.random.fold_in(arg_keys[2], 1), TOKENS // TOK_DEV)
    routes_turns = jax.random.permutation(jax.random.fold_in(arg_keys[2], 3), TOKENS // TOK_DEV)
    routes = jax.vmap(lambda own, number: assign_block(jax.random.fold_in(arg_keys[2], 2), own, number, TOK_DEV, EXPERTS, TOPK, CAP, 2))(routes_keys, routes_turns).reshape((TOKENS, TOPK))
    route_weights = jnp.clip(0.05 + 0.95 * jax.random.uniform(arg_keys[3], (TOKENS, TOPK), jnp.float32) ** level_of(arg_keys[3], (TOKENS, TOPK), ((0, 8),), -0.2, 0.2), 0.05, 1.0)
    w_gate = scatter_about(arg_keys[4], (EXPERTS, D, FF), (D // 9) ** -0.5, 0.25, ((0, 8), (2, 4)))
    w_up = scatter_about(arg_keys[5], (EXPERTS, D, FF), (D // 9) ** -0.5, 0.25, ((0, 8), (2, 4)))
    w_down = scatter_about(arg_keys[6], (EXPERTS, FF, D), (16 * FF) ** -0.5, 0.0234375, ((0, 8), (1, 4)))
    return dict(tokens=tokens, norm_gain=norm_gain, routes=routes, route_weights=route_weights, w_gate=w_gate, w_up=w_up, w_down=w_down)


def reference(tokens, norm_gain, routes, route_weights, w_gate, w_up, w_down):
    values = tokens.astype(jnp.float32)
    scale = lax.rsqrt(lax.optimization_barrier(jnp.mean(values * values, axis=1, keepdims=True)) + 1e-05)
    normed = (values * scale * norm_gain.astype(jnp.float32)[None, :]).astype(jnp.bfloat16)
    blocks = N_TP
    rows = tokens.shape[0]

    def one_expert(carry, expert):
        gate_pre = jnp.dot(normed, w_gate[expert], preferred_element_type=jnp.float32)
        up_pre = jnp.dot(normed, w_up[expert], preferred_element_type=jnp.float32)
        gated = jnp.minimum(gate_pre, 7.0)
        upper = jnp.clip(up_pre, -7.0, 7.0)
        hidden = ((upper + 1.0) * gated * jax.nn.sigmoid(1.702 * gated)).astype(jnp.bfloat16)
        width = hidden.shape[1] // blocks
        hidden_blocks = hidden.reshape(rows, blocks, width).astype(jnp.float32)
        down_blocks = w_down[expert].reshape(blocks, width, -1).astype(jnp.float32)
        parts = jnp.einsum('tbf,bfd->btd', hidden_blocks, down_blocks).astype(jnp.bfloat16)
        parts = lax.optimization_barrier(parts).astype(jnp.float32)
        result = lax.optimization_barrier(jnp.sum(parts, axis=0)).astype(jnp.bfloat16)
        result = lax.optimization_barrier(result).astype(jnp.float32)
        weight = lax.optimization_barrier(jnp.sum(jnp.where(routes == expert, route_weights, 0.0), axis=1))
        return (carry + weight[:, None] * result, None)
    start = jnp.zeros(tokens.shape, jnp.float32)
    total, _ = lax.scan(one_expert, start, jnp.arange(EXPERTS, dtype=jnp.int32))
    return total.astype(jnp.bfloat16)
```

```python
import functools

import jax
import jax.numpy as jnp
from jax import lax
from jax.experimental import pallas as pl
from jax.experimental.pallas import tpu as pltpu
from jax.sharding import PartitionSpec as P

MESH = pl.DeviceIdType.MESH
CORES = 2
EXTRA = 128
HALF_EXTRA = EXTRA // 2
SQUARES = HALF_EXTRA - 2


def flip(index, bits):
    bit = 1
    while bit <= bits:
        if bits & bit:
            index = index + bit - 2 * bit * ((index // bit) % 2)
        bit *= 2
    return index


def kernel(
    n_z, n_tp,
    tokens, gain, routes, route_weights, w_gate, w_up, w_down,
    out,
    gate_v, up_v, down_v, gathered, acc_gate, acc_up, hidden,
    pair_send, pair_recv, pair_own, tp_send, tp_recv, z_send, z_recv,
    w_sem, a_zs, a_zr, a_ts, a_tr, a_ps, a_pr, b_ps, b_pr, b_ts, b_tr, b_zs, b_zr,
):
    ep, tp = lax.axis_index("ep"), lax.axis_index("tp")
    z, core = ep // CORES, ep % CORES
    other = 1 - core
    rows, width = tokens.shape
    half = n_z * rows
    units = gate_v.shape[1]
    tile = min(256, units)
    out_tile = min(256, width)

    def block(zz):
        return pl.ds(pl.multiple_of((core * n_z + zz) * rows, rows), rows)

    def core_rows(cc):
        return pl.ds(pl.multiple_of(cc * half, half), half)

    def features(tt):
        return pl.ds(pl.multiple_of(tt * width, width), width)

    weight_copies = []
    for kt in range(n_tp):
        part = features(flip(tp, kt))
        for side, (hbm, vmem) in enumerate(((w_gate, gate_v), (w_up, up_v))):
            copy = pltpu.make_async_copy(
                hbm.at[0, part, :], vmem.at[part, :], w_sem.at[2 * kt + side]
            )
            copy.start()
            weight_copies.append(copy)
    down_copy = pltpu.make_async_copy(w_down.at[0], down_v, w_sem.at[2 * n_tp])
    down_copy.start()

    barrier = pltpu.get_barrier_semaphore()
    peers = [(flip(z, k) * CORES + core, tp) for k in range(1, n_z)]
    peers += [(ep, flip(tp, k)) for k in range(1, n_tp)]
    peers += [(z * CORES + other, tp)]
    for peer in peers:
        pl.semaphore_signal(barrier, inc=1, device_id=peer, device_id_type=MESH)

    values = tokens[...].astype(jnp.float32)
    squares = jnp.sum(values * values, axis=1, keepdims=True)
    lane = lax.broadcasted_iota(jnp.int32, (rows, EXTRA), 1)
    place = lane % HALF_EXTRA
    side_values = jnp.where(place == SQUARES, squares, 0.0)
    for k in range(routes.shape[1]):
        side_values += jnp.where(place == routes[:, k : k + 1], route_weights[:, k : k + 1], 0.0)
    high = side_values.astype(jnp.bfloat16).astype(jnp.float32)
    side_values = jnp.where(lane < HALF_EXTRA, high, side_values - high)
    gathered[tp, block(z), :width] = (values * gain[...].astype(jnp.float32)).astype(jnp.bfloat16)
    gathered[tp, block(z), width:] = side_values.astype(jnp.bfloat16)
    pl.semaphore_wait(barrier, len(peers))

    def remote(src, dst, send, recv, peer):
        return pltpu.make_async_remote_copy(
            src_ref=src, dst_ref=dst, send_sem=send, recv_sem=recv,
            device_id=peer, device_id_type=MESH,
        )

    def z_peer(k):
        return (flip(z, k) * CORES + core, tp)

    def tp_peer(k):
        return (ep, flip(tp, k))

    partner = (z * CORES + other, tp)
    sent = []

    def send(*args):
        copy = remote(*args)
        copy.start()
        sent.append(copy)

    mine = gathered.at[tp, block(z), :]
    for kz in range(n_z - 1, 0, -1):
        send(mine, mine, a_zs.at[kz], a_zr.at[kz], z_peer(kz))
    for kz in range(n_z):
        here = gathered.at[tp, block(flip(z, kz)), :]
        if kz > 0:
            remote(here, here, a_zs.at[kz], a_zr.at[kz], z_peer(kz)).wait_recv()
        for kt in range(1, n_tp):
            send(here, here, a_ts.at[kt, kz], a_tr.at[kt, kz], tp_peer(kt))

    def to_partner(kt):
        if kt > 0:
            for kz in range(n_z):
                there = gathered.at[flip(tp, kt), block(flip(z, kz)), :]
                remote(there, there, a_ts.at[kt, kz], a_tr.at[kt, kz], tp_peer(kt)).wait_recv()
        ours = gathered.at[flip(tp, kt), core_rows(core), :]
        send(ours, ours, a_ps.at[kt], a_pr.at[kt], partner)

    to_partner(0)
    for kt in range(n_tp):
        if kt + 1 < n_tp:
            to_partner(kt + 1)
        source = flip(tp, kt)
        theirs = gathered.at[source, core_rows(other), :]
        remote(theirs, theirs, a_ps.at[kt], a_pr.at[kt], partner).wait_recv()
        weight_copies[2 * kt].wait()
        weight_copies[2 * kt + 1].wait()

        @pl.loop(0, units // tile)
        def _(n):
            columns = pl.ds(pl.multiple_of(n * tile, tile), tile)
            left = gathered[source, :, :width]
            for vmem, acc in ((gate_v, acc_gate), (up_v, acc_up)):
                product = jnp.dot(
                    left, vmem[features(source), columns], preferred_element_type=jnp.float32
                )
                if kt > 0:
                    product += acc[:, columns]
                acc[:, columns] = product

    lanes = lax.broadcasted_iota(jnp.int32, (half, EXTRA), 1)
    for at, cc in enumerate((other, core)):
        group = core_rows(cc)
        total = jnp.zeros((half, EXTRA), jnp.float32)
        for kt in range(n_tp):
            total += gathered[kt, group, width:].astype(jnp.float32)
        picked = jnp.where(lanes % HALF_EXTRA == SQUARES, total, 0.0)
        mean = jnp.sum(picked, axis=1, keepdims=True) / (n_tp * width)
        scale = lax.rsqrt(mean + 1e-05)
        chosen = jnp.where(
            lanes % HALF_EXTRA == ep, gathered[tp, group, width:].astype(jnp.float32), 0.0
        )
        weight = jnp.sum(chosen, axis=1, keepdims=True)
        gated = jnp.minimum(acc_gate[group, :] * scale, 7.0)
        upper = jnp.clip(acc_up[group, :] * scale, -7.0, 7.0)
        values = (upper + 1.0) * gated * jax.nn.sigmoid(1.702 * gated)
        hidden[at * half : (at + 1) * half, :] = (values * weight).astype(jnp.bfloat16)

    down_copy.wait()

    def pair_sum(kt):
        remote(
            pair_send.at[kt], pair_recv.at[kt], b_ps.at[kt], b_pr.at[kt], partner
        ).wait_recv()
        total = pair_own[kt] + pair_recv[kt].astype(jnp.float32)
        if kt == 0:
            pair_own[0] = total
        else:
            tp_send[kt] = total.astype(jnp.bfloat16)

    order = list(range(n_tp - 1, -1, -1))
    for step, kt in enumerate(order):
        target = flip(tp, kt)

        @pl.loop(0, width // out_tile)
        def _(n):
            columns = pl.ds(pl.multiple_of(n * out_tile, out_tile), out_tile)
            from_column = pl.multiple_of(target * width + n * out_tile, out_tile)
            product = jnp.dot(
                hidden[...], down_v[:, pl.ds(from_column, out_tile)],
                preferred_element_type=jnp.float32,
            )
            pair_send[kt, :, columns] = product[:half].astype(jnp.bfloat16)
            pair_own[kt, :, columns] = product[half:]

        send(pair_send.at[kt], pair_recv.at[kt], b_ps.at[kt], b_pr.at[kt], partner)
        if step > 0:
            pair_sum(order[step - 1])
        if step == n_tp - 1:
            break

    def z_rows(kz):
        return pl.ds(pl.multiple_of(flip(z, kz) * rows, rows), rows)

    def tp_copy(kt, kz):
        return remote(
            tp_send.at[kt, z_rows(kz), :], tp_recv.at[kt, z_rows(kz), :],
            b_ts.at[kt, kz], b_tr.at[kt, kz], tp_peer(kt),
        )

    for kz in range(n_z - 1, -1, -1):
        for kt in range(n_tp - 1, 0, -1):
            copy = tp_copy(kt, kz)
            copy.start()
            sent.append(copy)
    pair_sum(0)
    final = None
    for kz in range(n_z - 1, -1, -1):
        total = pair_own[0, z_rows(kz), :]
        for kt in range(n_tp - 1, 0, -1):
            tp_copy(kt, kz).wait_recv()
            total += tp_recv[kt, z_rows(kz), :].astype(jnp.float32)
        if kz > 0:
            z_send[kz] = total.astype(jnp.bfloat16)
            send(z_send.at[kz], z_recv.at[kz], b_zs.at[kz], b_zr.at[kz], z_peer(kz))
        else:
            final = total
    for kz in range(n_z - 1, 0, -1):
        remote(z_send.at[kz], z_recv.at[kz], b_zs.at[kz], b_zr.at[kz], z_peer(kz)).wait_recv()
        final += z_recv[kz].astype(jnp.float32)
    out[...] = final.astype(jnp.bfloat16)
    for copy in sent:
        copy.wait_send()


def shards(n_ep, n_tp, tokens, norm_gain, routes, route_weights, w_gate, w_up, w_down):
    rows, width = tokens.shape
    depth, units = w_gate.shape[1:]
    n_z = n_ep // CORES
    half = n_z * rows
    everyone = n_ep * rows
    bf16, f32, dma = jnp.bfloat16, jnp.float32, pltpu.SemaphoreType.DMA
    vmem = pl.BlockSpec(memory_space=pltpu.VMEM)
    anywhere = pl.BlockSpec(memory_space=pl.ANY)
    return pl.pallas_call(
        functools.partial(kernel, n_z, n_tp),
        out_shape=jax.ShapeDtypeStruct((rows, width), bf16),
        in_specs=[vmem] * 4 + [anywhere] * 3,
        out_specs=vmem,
        scratch_shapes=[
            pltpu.VMEM((depth, units), bf16),
            pltpu.VMEM((depth, units), bf16),
            pltpu.VMEM((units, depth), bf16),
            pltpu.VMEM((n_tp, everyone, width + EXTRA), bf16),
            pltpu.VMEM((everyone, units), f32),
            pltpu.VMEM((everyone, units), f32),
            pltpu.VMEM((everyone, units), bf16),
            pltpu.VMEM((n_tp, half, width), bf16),
            pltpu.VMEM((n_tp, half, width), bf16),
            pltpu.VMEM((n_tp, half, width), f32),
            pltpu.VMEM((n_tp, half, width), bf16),
            pltpu.VMEM((n_tp, half, width), bf16),
            pltpu.VMEM((n_z, rows, width), bf16),
            pltpu.VMEM((n_z, rows, width), bf16),
            dma((2 * n_tp + 1,)),
            dma((n_z,)), dma((n_z,)),
            dma((n_tp, n_z)), dma((n_tp, n_z)),
            dma((n_tp,)), dma((n_tp,)),
            dma((n_tp,)), dma((n_tp,)),
            dma((n_tp, n_z)), dma((n_tp, n_z)),
            dma((n_z,)), dma((n_z,)),
        ],
        compiler_params=pltpu.CompilerParams(
            collective_id=0, has_side_effects=True, vmem_limit_bytes=60 * 1024 * 1024
        ),
    )(tokens, norm_gain.reshape(1, -1), routes, route_weights, w_gate, w_up, w_down)


def solution(mesh):
    placed = (
        P("ep", "tp"),
        P("tp"),
        P("ep", None),
        P("ep", None),
        P("ep", None, "tp"),
        P("ep", None, "tp"),
        P("ep", "tp", None),
    )
    return jax.shard_map(
        functools.partial(shards, mesh.shape["ep"], mesh.shape["tp"]),
        mesh=mesh, in_specs=placed, out_specs=P("ep", "tp"), check_vma=False,
    )
```

```python
import functools

import jax
import jax.numpy as jnp
from jax import lax
from jax.experimental import pallas as pl
from jax.experimental.pallas import tpu as pltpu
from jax.sharding import PartitionSpec as P

MESH = pl.DeviceIdType.MESH
CORES = 2
EXTRA = 128
HALF_EXTRA = EXTRA // 2
SQUARES = HALF_EXTRA - 2


def flip(index, bits):
    bit = 1
    while bit <= bits:
        if bits & bit:
            index = index + bit - 2 * bit * ((index // bit) % 2)
        bit *= 2
    return index


def kernel(
    n_z, n_tp,
    tokens_in, gain_in, routes_in, route_weights_in, w_gate, w_up, w_down,
    out,
    tokens, gain, routes, route_weights,
    gate_v, up_v, down_v, gathered, acc_gate, acc_up, hidden,
    pair_send, pair_recv, pair_own, tp_send, tp_recv, z_send, z_recv,
    in_sem, w_sem, a_zs, a_zr, a_ts, a_tr, a_ps, a_pr, b_ps, b_pr, b_ts, b_tr, b_zs, b_zr,
):
    ep, tp = lax.axis_index("ep"), lax.axis_index("tp")
    z, core = ep // CORES, ep % CORES
    other = 1 - core
    rows, width = tokens.shape
    half = n_z * rows
    units = gate_v.shape[1]
    tile = min(256, units)
    out_tile = min(256, width)

    def block(zz):
        return pl.ds(pl.multiple_of((core * n_z + zz) * rows, rows), rows)

    def core_rows(cc):
        return pl.ds(pl.multiple_of(cc * half, half), half)

    def features(tt):
        return pl.ds(pl.multiple_of(tt * width, width), width)

    barrier = pltpu.get_barrier_semaphore()
    peers = [(flip(z, k) * CORES + core, tp) for k in range(1, n_z)]
    peers += [(ep, flip(tp, k)) for k in range(1, n_tp)]
    peers += [(z * CORES + other, tp)]
    for peer in peers:
        pl.semaphore_signal(barrier, inc=1, device_id=peer, device_id_type=MESH)

    small = (
        (tokens_in, tokens), (gain_in, gain), (routes_in, routes),
        (route_weights_in, route_weights),
    )
    small_copies = [
        pltpu.make_async_copy(src, dst, in_sem.at[i]) for i, (src, dst) in enumerate(small)
    ]
    for copy in small_copies:
        copy.start()
    weight_copies = []
    for kt in range(n_tp):
        part = features(flip(tp, kt))
        for side, (hbm, vmem) in enumerate(((w_gate, gate_v), (w_up, up_v))):
            copy = pltpu.make_async_copy(
                hbm.at[0, part, :], vmem.at[part, :], w_sem.at[2 * kt + side]
            )
            copy.start()
            weight_copies.append(copy)
    down_copy = pltpu.make_async_copy(w_down.at[0], down_v, w_sem.at[2 * n_tp])
    down_copy.start()

    for copy in small_copies:
        copy.wait()
    values = tokens[...].astype(jnp.float32)
    squares = jnp.sum(values * values, axis=1, keepdims=True)
    lane = lax.broadcasted_iota(jnp.int32, (rows, EXTRA), 1)
    place = lane % HALF_EXTRA
    side_values = jnp.where(place == SQUARES, squares, 0.0)
    diagonal = lax.broadcasted_iota(jnp.int32, (rows, rows), 0) == lax.broadcasted_iota(
        jnp.int32, (rows, rows), 1
    )
    for k in range(routes.shape[0]):
        expert = jnp.sum(jnp.where(diagonal, routes[k : k + 1, :], 0), axis=1, keepdims=True)
        weight = jnp.sum(
            jnp.where(diagonal, route_weights[k : k + 1, :], 0.0), axis=1, keepdims=True
        )
        side_values += jnp.where(place == expert, weight, 0.0)
    high = side_values.astype(jnp.bfloat16).astype(jnp.float32)
    side_values = jnp.where(lane < HALF_EXTRA, high, side_values - high)
    gathered[tp, block(z), :width] = (values * gain[...].astype(jnp.float32).reshape(1, width)).astype(jnp.bfloat16)
    gathered[tp, block(z), width:] = side_values.astype(jnp.bfloat16)
    pl.semaphore_wait(barrier, len(peers))

    def remote(src, dst, send, recv, peer):
        return pltpu.make_async_remote_copy(
            src_ref=src, dst_ref=dst, send_sem=send, recv_sem=recv,
            device_id=peer, device_id_type=MESH,
        )

    def z_peer(k):
        return (flip(z, k) * CORES + core, tp)

    def tp_peer(k):
        return (ep, flip(tp, k))

    partner = (z * CORES + other, tp)
    sent = []

    def send(*args):
        copy = remote(*args)
        copy.start()
        sent.append(copy)

    mine = gathered.at[tp, block(z), :]
    for kz in range(n_z - 1, 0, -1):
        send(mine, mine, a_zs.at[kz], a_zr.at[kz], z_peer(kz))
    for kz in range(n_z):
        here = gathered.at[tp, block(flip(z, kz)), :]
        if kz > 0:
            remote(here, here, a_zs.at[kz], a_zr.at[kz], z_peer(kz)).wait_recv()
        for kt in range(1, n_tp):
            send(here, here, a_ts.at[kt, kz], a_tr.at[kt, kz], tp_peer(kt))

    def to_partner(kt):
        if kt > 0:
            for kz in range(n_z):
                there = gathered.at[flip(tp, kt), block(flip(z, kz)), :]
                remote(there, there, a_ts.at[kt, kz], a_tr.at[kt, kz], tp_peer(kt)).wait_recv()
        ours = gathered.at[flip(tp, kt), core_rows(core), :]
        send(ours, ours, a_ps.at[kt], a_pr.at[kt], partner)

    to_partner(0)
    passed = 1
    for kt in range(n_tp):
        while passed < n_tp and passed <= (0, 2)[min(kt, 1)] + max(0, kt - 1):
            to_partner(passed)
            passed += 1
        source = flip(tp, kt)
        theirs = gathered.at[source, core_rows(other), :]
        remote(theirs, theirs, a_ps.at[kt], a_pr.at[kt], partner).wait_recv()
        weight_copies[2 * kt].wait()
        weight_copies[2 * kt + 1].wait()

        @pl.loop(0, units // tile)
        def _(n):
            columns = pl.ds(pl.multiple_of(n * tile, tile), tile)
            left = gathered[source, :, :width]
            for vmem, acc in ((gate_v, acc_gate), (up_v, acc_up)):
                product = jnp.dot(
                    left, vmem[features(source), columns], preferred_element_type=jnp.float32
                )
                if kt > 0:
                    product += acc[:, columns]
                acc[:, columns] = product

    lanes = lax.broadcasted_iota(jnp.int32, (half, EXTRA), 1)
    for at, cc in enumerate((other, core)):
        group = core_rows(cc)
        total = jnp.zeros((half, EXTRA), jnp.float32)
        for kt in range(n_tp):
            total += gathered[kt, group, width:].astype(jnp.float32)
        picked = jnp.where(lanes % HALF_EXTRA == SQUARES, total, 0.0)
        mean = jnp.sum(picked, axis=1, keepdims=True) / (n_tp * width)
        scale = lax.rsqrt(mean + 1e-05)
        chosen = jnp.where(
            lanes % HALF_EXTRA == ep, gathered[tp, group, width:].astype(jnp.float32), 0.0
        )
        weight = jnp.sum(chosen, axis=1, keepdims=True)
        gated = jnp.minimum(acc_gate[group, :] * scale, 7.0)
        upper = jnp.clip(acc_up[group, :] * scale, -7.0, 7.0)
        values = (upper + 1.0) * gated * jax.nn.sigmoid(1.702 * gated)
        hidden[at * half : (at + 1) * half, :] = (values * weight).astype(jnp.bfloat16)

    down_copy.wait()

    def pair_sum(kt):
        remote(
            pair_send.at[kt], pair_recv.at[kt], b_ps.at[kt], b_pr.at[kt], partner
        ).wait_recv()
        total = pair_own[kt] + pair_recv[kt].astype(jnp.float32)
        if kt == 0:
            pair_own[0] = total
        else:
            tp_send[kt] = total.astype(jnp.bfloat16)

    def z_rows(kz):
        return pl.ds(pl.multiple_of(flip(z, kz) * rows, rows), rows)

    def tp_copy(kt, kz):
        return remote(
            tp_send.at[kt, z_rows(kz), :], tp_recv.at[kt, z_rows(kz), :],
            b_ts.at[kt, kz], b_tr.at[kt, kz], tp_peer(kt),
        )

    def send_sum(kt, kz):
        copy = tp_copy(kt, kz)
        copy.start()
        sent.append(copy)

    order = list(range(n_tp - 1, -1, -1))
    late = order[-3:-1]
    for step, kt in enumerate(order):
        target = flip(tp, kt)

        @pl.loop(0, width // out_tile)
        def _(n):
            columns = pl.ds(pl.multiple_of(n * out_tile, out_tile), out_tile)
            from_column = pl.multiple_of(target * width + n * out_tile, out_tile)
            product = jnp.dot(
                hidden[...], down_v[:, pl.ds(from_column, out_tile)],
                preferred_element_type=jnp.float32,
            )
            pair_send[kt, :, columns] = product[:half].astype(jnp.bfloat16)
            pair_own[kt, :, columns] = product[half:]

        send(pair_send.at[kt], pair_recv.at[kt], b_ps.at[kt], b_pr.at[kt], partner)
        if step > 0:
            done = order[step - 1]
            pair_sum(done)
            if done not in late:
                for kz in range(n_z - 1, -1, -1):
                    send_sum(done, kz)

    for kz in range(n_z - 1, -1, -1):
        for kt in late:
            send_sum(kt, kz)
    pair_sum(0)
    final = None
    for kz in range(n_z - 1, -1, -1):
        total = pair_own[0, z_rows(kz), :]
        for kt in range(n_tp - 1, 0, -1):
            tp_copy(kt, kz).wait_recv()
            total += tp_recv[kt, z_rows(kz), :].astype(jnp.float32)
        if kz > 0:
            z_send[kz] = total.astype(jnp.bfloat16)
            send(z_send.at[kz], z_recv.at[kz], b_zs.at[kz], b_zr.at[kz], z_peer(kz))
        else:
            final = total
    for kz in range(n_z - 1, 0, -1):
        remote(z_send.at[kz], z_recv.at[kz], b_zs.at[kz], b_zr.at[kz], z_peer(kz)).wait_recv()
        final += z_recv[kz].astype(jnp.float32)
    out[...] = final.astype(jnp.bfloat16)
    for copy in sent:
        copy.wait_send()


def shards(n_ep, n_tp, tokens, norm_gain, routes, route_weights, w_gate, w_up, w_down):
    rows, width = tokens.shape
    depth, units = w_gate.shape[1:]
    n_z = n_ep // CORES
    half = n_z * rows
    everyone = n_ep * rows
    bf16, f32, dma = jnp.bfloat16, jnp.float32, pltpu.SemaphoreType.DMA
    vmem = pl.BlockSpec(memory_space=pltpu.VMEM)
    anywhere = pl.BlockSpec(memory_space=pl.ANY)
    return pl.pallas_call(
        functools.partial(kernel, n_z, n_tp),
        out_shape=pltpu.VMEM((rows, width), bf16),
        in_specs=[anywhere] * 7,
        out_specs=vmem,
        scratch_shapes=[
            pltpu.VMEM((rows, width), bf16),
            pltpu.VMEM((width,), bf16),
            pltpu.VMEM(routes.T.shape, routes.dtype),
            pltpu.VMEM(routes.T.shape, f32),
            pltpu.VMEM((depth, units), bf16),
            pltpu.VMEM((depth, units), bf16),
            pltpu.VMEM((units, depth), bf16),
            pltpu.VMEM((n_tp, everyone, width + EXTRA), bf16),
            pltpu.VMEM((everyone, units), f32),
            pltpu.VMEM((everyone, units), f32),
            pltpu.VMEM((everyone, units), bf16),
            pltpu.VMEM((n_tp, half, width), bf16),
            pltpu.VMEM((n_tp, half, width), bf16),
            pltpu.VMEM((n_tp, half, width), f32),
            pltpu.VMEM((n_tp, half, width), bf16),
            pltpu.VMEM((n_tp, half, width), bf16),
            pltpu.VMEM((n_z, rows, width), bf16),
            pltpu.VMEM((n_z, rows, width), bf16),
            dma((4,)),
            dma((2 * n_tp + 1,)),
            dma((n_z,)), dma((n_z,)),
            dma((n_tp, n_z)), dma((n_tp, n_z)),
            dma((n_tp,)), dma((n_tp,)),
            dma((n_tp,)), dma((n_tp,)),
            dma((n_tp, n_z)), dma((n_tp, n_z)),
            dma((n_z,)), dma((n_z,)),
        ],
        compiler_params=pltpu.CompilerParams(
            collective_id=0, has_side_effects=True, vmem_limit_bytes=60 * 1024 * 1024
        ),
    )(tokens, norm_gain, routes.T, route_weights.T, w_gate, w_up, w_down)


def solution(mesh):
    placed = (
        P("ep", "tp"),
        P("tp"),
        P("ep", None),
        P("ep", None),
        P("ep", None, "tp"),
        P("ep", None, "tp"),
        P("ep", "tp", None),
    )
    return jax.shard_map(
        functools.partial(shards, mesh.shape["ep"], mesh.shape["tp"]),
        mesh=mesh, in_specs=placed, out_specs=P("ep", "tp"), check_vma=False,
    )
```
